128 devices in a mesh: ep: 64 (over z, y, x), tp: 2 (over core).
Axes of the slice: x: 4, y: 4, z: 4, core: 2. Of those that a mesh axis runs over, the one named last changes fastest.
Arguments:
- residual: bfloat16 [1024, 4096], P(('ep', 'tp')), may hold values from -6 to 6
- lengths: int32 [1024], P(('ep', 'tp')), may hold values from 128 to 1024
- latent_cache: bfloat16 [1024, 1024, 512], P(('ep', 'tp'))
- rope_cache: bfloat16 [1024, 1024, 64], P(('ep', 'tp')), may hold values from -6 to 6
- route_ids: int32 [1024, 2], P(('ep', 'tp')), may hold values from 0 to 7, all different within a row; in each aligned block of 8 rows (0 to 7, 8 to 15, ...) at most 3 rows name the same one
- route_scores: bfloat16 [1024, 2], P(('ep', 'tp')), may hold values from -6 to 6
- norm_first: float32 [4096], replicated, may hold values from 0.1 to 1.9
- norm_second: float32 [4096], replicated, may hold values from 0.1 to 1.9
- query_gain: float32 [1024], replicated, may hold values from 0.1 to 1.9
- latent_gain: float32 [512], replicated, may hold values from 0.1 to 1.9
- query_down: bfloat16 [4096, 1024], P(('ep', 'tp')), may hold values from -0.09375 to 0.09375
- latent_down: bfloat16 [4096, 512], P(('ep', 'tp')), may hold values from -0.09375 to 0.09375
- rope_down: bfloat16 [4096, 64], replicated, may hold values from -0.09375 to 0.09375
- query_latent: bfloat16 [1024, 16384], P(None, ('ep', 'tp')), may hold values from -0.1875 to 0.1875
- query_rope: bfloat16 [1024, 2048], P(None, ('ep', 'tp')), may hold values from -0.1875 to 0.1875
- value_up: bfloat16 [512, 32, 128], replicated, may hold values from -1 to 1
- output_weight: bfloat16 [4096, 4096], P(None, ('ep', 'tp')), may hold values from -0.09375 to 0.09375
- expert_gate: bfloat16 [4096, 57344], P(None, ('ep', 'tp')), may hold values from -0.09375 to 0.09375
- expert_up: bfloat16 [4096, 57344], P(None, ('ep', 'tp')), may hold values from -0.09375 to 0.09375
- expert_down: bfloat16 [57344, 4096], P(('ep', 'tp')), may hold values from -0.125 to 0.125
Outputs:
- layer_out: bfloat16 [1024, 4096], P(('ep', 'tp'))
- new_latent: bfloat16 [1024, 512], P(('ep', 'tp'))
- new_rope: bfloat16 [1024, 64], P(('ep', 'tp'))
The draws below stay inside these ranges and needn't reach their ends.
Inputs may be any that keep to these rules, and one draw needn't show every extreme that they name: `route_ids`: each row names 2 different experts. Within the rows of one device (aligned blocks of 8 rows) no expert is named more than 3 times; in every draw some expert is named exactly 3 times in some blocks. `lengths`: A sequence's cached positions are 0 to its length - 1; the new token stands at position length.
All inputs are finite; a program needn't handle non-finite values.
Results may differ from the reference program's by a relative error of at most 0.014.
The reference program's roundings to bfloat16 on the way count: a program that leaves them out, or rounds other values in their place, can miss the bound.
Values may be sent and summed in bfloat16 or wider, within the bound.
A program may use at most 128 MiB of HBM per device.

```python
import math
import jax
import jax.numpy as jnp
import numpy as np
from jax import lax

D = 4096
HEADS = 32
Q_RANK = 1024
KV_RANK = 512
ROPE = 64
NOPE = 128
VDIM = 128
EXPERTS = 8
D_EXPERT = 7168
TOP = 2
SEQ_DEV = 8
CACHE = 1024
TOKENS = 1024
CAP = 3


def draw_latent_cache(key, part):
    values_drawn = jax.random.normal(jax.random.fold_in(key, 11), (TOKENS, CACHE, KV_RANK), jnp.float32)
    return values_drawn.astype(jnp.bfloat16)


def plant(values, key, least, high):
    longest = values.shape.index(max(values.shape))
    spots = []
    for shift in (0, 1):
        where = [jax.random.randint(jax.random.fold_in(key, axis), (), 0, length) for axis, length in enumerate(values.shape)]
        where[longest] = (where[longest] + shift) % values.shape[longest]
        spots.append(tuple(where))
    return values.at[spots[0]].set(least).at[spots[1]].set(high)


def levels(key, shape, cuts, least, top_value):
    gain, own = 1.0, jax.random.fold_in(key, 6)
    for position, blocks in cuts:
        heights = jnp.exp(jax.random.uniform(jax.random.fold_in(own, position), (blocks,), jnp.float32, least / len(cuts), top_value / len(cuts)))
        gain = gain * jnp.repeat(heights, shape[position] // blocks).reshape([-1 if axis == position else 1 for axis in range(len(shape))])
    return gain


def routed_block(stream_key, own, number, rows, amount, top, most, skew):
    ranking = jax.random.permutation(stream_key, amount)
    packed, common = load_shares(amount, rows * top, most, skew, True), load_shares(amount, rows * top, most, skew, False)
    places = jnp.arange(amount)

    def named(tallies, turn):
        used = int((tallies > 0).sum())
        fixed = max(1, used // 4)
        moved = fixed + (places - fixed + turn * (used - fixed)) % max(1, amount - fixed)
        return jnp.zeros((amount,), jnp.int32).at[ranking[jnp.where(places < fixed, places, moved)]].set(jnp.asarray(tallies, jnp.int32))

    tallies = jnp.where(number % 4 == 0, named(packed, number // 4), named(common, number - number // 4 - 1))
    mixed = jax.random.permutation(jax.random.fold_in(own, 3), amount)
    giver, receiver = mixed[0:amount // 2 * 2:2], mixed[1:amount // 2 * 2:2]
    room = jnp.minimum(tallies[giver] - 1, most - tallies[receiver]) // 2
    room = jnp.where((giver == ranking[0]) | (receiver == ranking[0]) | (tallies[receiver] == 0), 0, jnp.maximum(room, 0))
    moved = jax.random.randint(jax.random.fold_in(own, 4), (amount // 2,), 0, 1 << 20) % (room + 1)
    tallies = tallies.at[giver].add(-moved).at[receiver].add(moved)
    members = jnp.searchsorted(jnp.cumsum(tallies), jnp.arange(rows * top), side="right").astype(jnp.int32)
    table = members.reshape(top, rows).T
    table = table[jax.random.permutation(jax.random.fold_in(own, 1), rows)]
    turn = jax.random.randint(jax.random.fold_in(own, 2), (rows, 1), 0, top)
    return jnp.take_along_axis(table, (jnp.arange(top)[None, :] + turn) % top, axis=1)


def load_shares(number_of, total, most, slope, full):
    weights = [(1 << 20) // math.isqrt(grade ** slope) + 1 for grade in range(1, number_of + 1)]
    largest = most if full else min(most, max(-(-total // number_of), total * weights[0] // sum(weights)))
    least = 1 if total - largest >= number_of - 1 else 0
    given, rest = [largest] + [least] * (number_of - 1), total - largest - least * (number_of - 1)
    while rest > 0:
        candidates = [i for i in range(1, number_of) if given[i] < largest] or [i for i in range(1, number_of) if given[i] < most]
        pool, left = sum([weights[i] for i in candidates]), rest
        for i in candidates:
            more = min(most - given[i], max(1, left * weights[i] // pool), rest)
            given[i] = given[i] + more
            rest = rest - more
    return np.array(given)


def centred(stream_key, extent, width, bound, split=(), held_as=jnp.bfloat16):
    gain = levels(stream_key, extent, split, -0.22, 0.18) if split else 1.0
    array = jax.random.normal(stream_key, extent, jnp.float32) * width * gain
    return jnp.minimum(jnp.maximum(array, -bound), bound).astype(held_as)


def setup_inputs(seed: int = 0) -> dict:
    arg_keys = jax.random.split(jax.random.key(seed), 21)
    residual = centred(arg_keys[0], (TOKENS, D), 1.0, 6.0, ((0, 128),))
    lengths = plant(jax.random.randint(arg_keys[1], (TOKENS,), CACHE // 8, CACHE + 1), jax.random.fold_in(arg_keys[1], 1), CACHE // 8, CACHE).astype(jnp.int32)
    latent_cache = draw_latent_cache(jax.random.fold_in(arg_keys[20], 71), 0)
    rope_cache = centred(arg_keys[3], (TOKENS, CACHE, ROPE), 1.0, 6.0, ((0, 128),))
    route_ids_keys = jax.random.split(jax.random.fold_in(arg_keys[4], 1), TOKENS // SEQ_DEV)
    route_ids_turns = jax.random.permutation(jax.random.fold_in(arg_keys[4], 3), TOKENS // SEQ_DEV)
    route_ids = jax.vmap(lambda own, number: routed_block(jax.random.fold_in(arg_keys[4], 2), own, number, SEQ_DEV, EXPERTS, TOP, CAP, 2))(route_ids_keys, route_ids_turns).reshape((TOKENS, TOP))
    route_scores = centred(arg_keys[5], (TOKENS, TOP), 1.5, 6.0, ((0, 128),))
    norm_first = jnp.clip(1.0 + 0.18 * jax.random.normal(arg_keys[6], (D,), jnp.float32), 0.1, 1.9)
    norm_second = jnp.clip(1.0 + 0.18 * jax.random.normal(arg_keys[7], (D,), jnp.float32), 0.1, 1.9)
    query_gain = jnp.clip(1.0 + 0.18 * jax.random.normal(arg_keys[8], (Q_RANK,), jnp.float32), 0.1, 1.9)
    latent_gain = jnp.clip(1.0 + 0.18 * jax.random.normal(arg_keys[9], (KV_RANK,), jnp.float32), 0.1, 1.9)
    query_down = centred(arg_keys[10], (D, Q_RANK), D ** -0.5, 0.09375, ((0, 128),))
    latent_down = centred(arg_keys[11], (D, KV_RANK), D ** -0.5, 0.09375, ((0, 128),))
    rope_down = centred(arg_keys[12], (D, ROPE), D ** -0.5, 0.09375)
    query_latent = centred(arg_keys[13], (Q_RANK, HEADS * KV_RANK), Q_RANK ** -0.5, 0.1875, ((1, 128),))
    query_rope = centred(arg_keys[14], (Q_RANK, HEADS * ROPE), Q_RANK ** -0.5, 0.1875, ((1, 128),))
    value_up = centred(arg_keys[15], (KV_RANK, HEADS, VDIM), (KV_RANK // 16) ** -0.5, 1.0)
    output_weight = centred(arg_keys[16], (HEADS * VDIM, D), (HEADS * VDIM) ** -0.5, 0.09375, ((1, 128),))
    expert_gate = centred(arg_keys[17], (D, EXPERTS * D_EXPERT), D ** -0.5, 0.09375, ((1, 128),))
    expert_up = centred(arg_keys[18], (D, EXPERTS * D_EXPERT), D ** -0.5, 0.09375, ((1, 128),))
    expert_down = centred(arg_keys[19], (EXPERTS * D_EXPERT, D), (D_EXPERT // 4) ** -0.5, 0.125, ((0, 128),))
    return dict(residual=residual, lengths=lengths, latent_cache=latent_cache, rope_cache=rope_cache, route_ids=route_ids, route_scores=route_scores, norm_first=norm_first, norm_second=norm_second, query_gain=query_gain, latent_gain=latent_gain, query_down=query_down, latent_down=latent_down, rope_down=rope_down, query_latent=query_latent, query_rope=query_rope, value_up=value_up, output_weight=output_weight, expert_gate=expert_gate, expert_up=expert_up, expert_down=expert_down)


epsilon = 1e-06
rope_base = 10000.0

def normalize(values_in, gain_row):
    return values_in * lax.rsqrt(lax.optimization_barrier(jnp.mean(values_in * values_in, axis=-1, keepdims=True)) + epsilon) * gain_row.astype(jnp.float32)

def rotate(values_in, turns):
    half_width = values_in.shape[-1] // 2
    front_half = values_in[..., :half_width]
    back_half = values_in[..., half_width:]
    cosine = jnp.cos(turns)
    sine_part = jnp.sin(turns)
    return jnp.concatenate([front_half * cosine - back_half * sine_part, front_half * sine_part + back_half * cosine], axis=-1)

def rotary_angles(positions, rotary_width):
    inverse = rope_base ** (-jnp.arange(0, rotary_width, 2, dtype=jnp.float32) / rotary_width)
    return positions.astype(jnp.float32)[:, None] * inverse[None, :]

def slot_tables(route_block):
    experts = jnp.arange(EXPERTS, dtype=jnp.int32)
    onehot = (route_block[..., None] == experts).astype(jnp.int32)
    earlier = jnp.cumsum(onehot, axis=-2) - onehot
    slot_rank = lax.optimization_barrier(jnp.sum(earlier * onehot, axis=-1))
    places = jnp.arange(CAP, dtype=jnp.int32)
    return onehot[..., None] * (slot_rank[..., None, None] == places).astype(jnp.int32)

def owner_table(sequences):
    assign = sequences * TOP
    return (jnp.arange(assign, dtype=jnp.int32)[None, :] // TOP == jnp.arange(sequences, dtype=jnp.int32)[:, None]).astype(jnp.float32)

def attend(operands):
    query_latents, query_rotary, latent_cache, rope_cache, new_latent, new_rope, lengths = operands
    score_scale = (NOPE + ROPE) ** (-0.5)
    latents_wide = latent_cache.astype(jnp.float32)
    query_wide = query_latents.astype(jnp.float32)
    rotary_wide = query_rotary.astype(jnp.float32)
    cache_scores = (jnp.einsum('shl,spl->shp', query_wide, latents_wide) + jnp.einsum('shr,spr->shp', rotary_wide, rope_cache.astype(jnp.float32))) * score_scale
    new_scores = (jnp.einsum('shl,sl->sh', query_wide, new_latent.astype(jnp.float32)) + jnp.einsum('shr,sr->sh', rotary_wide, new_rope.astype(jnp.float32))) * score_scale
    visible = jnp.arange(CACHE, dtype=jnp.int32)[None, :] < lengths[:, None]
    cache_scores = jnp.where(visible[:, None, :], cache_scores, -jnp.inf)
    row_top = jnp.maximum(lax.optimization_barrier(jnp.max(cache_scores, axis=-1)), new_scores)
    cache_terms = jnp.exp(cache_scores - row_top[..., None])
    new_term = jnp.exp(new_scores - row_top)
    denominator = lax.optimization_barrier(jnp.sum(cache_terms, axis=-1)) + new_term
    cache_probs = (cache_terms / denominator[..., None]).astype(jnp.bfloat16)
    new_probs = (new_term / denominator).astype(jnp.bfloat16)
    mixture = jnp.einsum('shp,spl->shl', cache_probs.astype(jnp.float32), latents_wide)
    mixture = mixture + new_probs.astype(jnp.float32)[..., None] * new_latent.astype(jnp.float32)[:, None, :]
    return mixture.astype(jnp.bfloat16)

def run_expert(operands):
    slot_rows, gate_block, up_block, down_block = operands
    flat_rows = slot_rows.reshape(-1, D)
    gate_part = jnp.dot(flat_rows, gate_block, preferred_element_type=jnp.float32)
    up_part = jnp.dot(flat_rows, up_block, preferred_element_type=jnp.float32)
    hidden = (jax.nn.silu(gate_part) * up_part).astype(jnp.bfloat16)
    return jnp.dot(hidden, down_block, preferred_element_type=jnp.float32).reshape(slot_rows.shape)

def reference(residual, lengths, latent_cache, rope_cache, route_ids, route_scores, norm_first, norm_second, query_gain, latent_gain, query_down, latent_down, rope_down, query_latent, query_rope, value_up, output_weight, expert_gate, expert_up, expert_down):
    stream = residual.astype(jnp.float32)
    normed = normalize(stream, norm_first).astype(jnp.bfloat16)
    query_part = jnp.dot(normed, query_down, preferred_element_type=jnp.float32)
    latent_part = jnp.dot(normed, latent_down, preferred_element_type=jnp.float32)
    query_small = normalize(query_part, query_gain).astype(jnp.bfloat16)
    new_latent = normalize(latent_part, latent_gain).astype(jnp.bfloat16)
    turns = rotary_angles(lengths, ROPE)
    new_rope = rotate(jnp.dot(normed, rope_down, preferred_element_type=jnp.float32), turns).astype(jnp.bfloat16)
    query_lat = jnp.dot(query_small, query_latent, preferred_element_type=jnp.float32).astype(jnp.bfloat16)
    query_lat = query_lat.reshape(TOKENS, HEADS, KV_RANK)
    query_pe = jnp.dot(query_small, query_rope, preferred_element_type=jnp.float32).astype(jnp.bfloat16)
    query_pe = query_pe.reshape(TOKENS, HEADS, ROPE)
    query_rot = rotate(query_pe.astype(jnp.float32), turns[:, None, :]).astype(jnp.bfloat16)
    blocks = TOKENS // SEQ_DEV

    def by_blocks(array_in):
        return array_in.reshape((blocks, SEQ_DEV) + array_in.shape[1:])
    mixture = lax.map(attend, tuple((by_blocks(item) for item in (query_lat, query_rot, latent_cache, rope_cache, new_latent, new_rope, lengths))))
    mixture = mixture.reshape(TOKENS, HEADS, KV_RANK)
    values = jnp.einsum('thl,lhv->thv', mixture.astype(jnp.float32), value_up.astype(jnp.float32))
    values = values.astype(jnp.bfloat16).reshape(TOKENS, HEADS * VDIM)
    attended = jnp.dot(values, output_weight, preferred_element_type=jnp.float32).astype(jnp.bfloat16)
    after_attention = stream + attended.astype(jnp.float32)
    second = normalize(after_attention, norm_second).astype(jnp.bfloat16)
    weights = jax.nn.softmax(route_scores.astype(jnp.float32), axis=-1)
    matches = slot_tables(route_ids.reshape(blocks, SEQ_DEV * TOP)).astype(jnp.float32)
    owners = owner_table(SEQ_DEV)
    picker = jnp.einsum('baec,sa->becs', matches, owners)
    slot_rows = jnp.einsum('becs,bsd->ebcd', picker, by_blocks(second).astype(jnp.float32), precision=lax.Precision.HIGHEST).astype(jnp.bfloat16)
    gate_blocks = expert_gate.reshape(D, EXPERTS, D_EXPERT).transpose(1, 0, 2)
    up_blocks = expert_up.reshape(D, EXPERTS, D_EXPERT).transpose(1, 0, 2)
    down_blocks = expert_down.reshape(EXPERTS, D_EXPERT, D)
    expert_outs = lax.map(run_expert, (slot_rows, gate_blocks, up_blocks, down_blocks))
    combine_weights = matches * weights.reshape(blocks, SEQ_DEV * TOP)[:, :, None, None]
    token_weights = jnp.einsum('baec,sa->bsec', combine_weights, owners, precision=lax.Precision.HIGHEST)
    routed = jnp.einsum('bsec,ebcd->bsd', token_weights, expert_outs, precision=lax.Precision.HIGHEST)
    layer_out = (after_attention + routed.reshape(TOKENS, D)).astype(jnp.bfloat16)
    return (layer_out, new_latent, new_rope)
```

```python
import jax
import jax.numpy as jnp
from jax import lax
from jax.experimental import pallas as pl
from jax.experimental.pallas import tpu as pltpu
from jax.sharding import Mesh
from jax.sharding import PartitionSpec as P

ROPE = 64
NOPE = 128
EXPERTS = 8
TOP = 2
CAP = 3
EP_TP = ("ep_0", "ep_1", "ep_2", "tp")
MESH = pl.DeviceIdType.MESH
HID = 448
F32 = jnp.float32
BF16 = jnp.bfloat16


epsilon = 1e-06
rope_base = 10000.0


def cut_along(shard, dim, peers):
    before, after = (shard.shape[:dim], shard.shape[dim + 1 :])
    return jnp.moveaxis(shard.reshape(*before, peers, -1, *after), dim, 0)


def sent_and_summed(shard, axis, dim):
    parts = cut_along(shard, dim, lax.axis_size(axis))
    arrived = lax.all_to_all(parts, axis, split_axis=0, concat_axis=0, tiled=True)
    return arrived.sum(axis=0)


def sum_by_axis(shard, axes, dim):
    far, near = axes
    parts = cut_along(shard, dim, lax.axis_size(far))
    nearer = sent_and_summed(parts, near, dim + 1)
    arrived = lax.all_to_all(nearer, far, split_axis=0, concat_axis=0, tiled=True)
    return arrived.sum(axis=0)


def sent_to_all(shard, axis):
    peers = lax.axis_size(axis)
    return lax.all_to_all(
        jnp.broadcast_to(shard[None], (peers, *shard.shape)), axis, 0, 0, tiled=True
    )


def in_order(parts, dim):
    shape = list(parts.shape[1:])
    shape[dim] *= parts.shape[0]
    return jnp.moveaxis(parts, 0, dim).reshape(shape)


def gathered_by_axis(shard, axes, dim):
    far, near = axes
    parts = sent_to_all(sent_to_all(shard, far), near)
    return in_order(parts.swapaxes(0, 1).reshape(-1, *shard.shape), dim)


def normalize(values_in, gain_row):
    return (
        values_in
        * lax.rsqrt(jnp.mean(values_in * values_in, axis=-1, keepdims=True) + epsilon)
        * gain_row
    )


def rotate(values_in, turns):
    half_width = values_in.shape[-1] // 2
    front_half = values_in[..., :half_width]
    back_half = values_in[..., half_width:]
    cosine = jnp.cos(turns)
    sine_part = jnp.sin(turns)
    return jnp.concatenate(
        [front_half * cosine - back_half * sine_part, front_half * sine_part + back_half * cosine],
        axis=-1,
    )


def rotary_angles(positions, rotary_width):
    inverse = rope_base ** (-jnp.arange(0, rotary_width, 2, dtype=jnp.float32) / rotary_width)
    return positions.astype(jnp.float32)[:, None] * inverse[None, :]


def slot_tables(route_block):
    experts = jnp.arange(EXPERTS, dtype=jnp.int32)
    onehot = (route_block[..., None] == experts).astype(jnp.int32)
    earlier = jnp.cumsum(onehot, axis=-2) - onehot
    slot_rank = jnp.sum(earlier * onehot, axis=-1)
    places = jnp.arange(CAP, dtype=jnp.int32)
    return onehot[..., None] * (slot_rank[..., None, None] == places).astype(jnp.int32)


def owner_table(sequences):
    assign = sequences * TOP
    return (
        jnp.arange(assign, dtype=jnp.int32)[None, :] // TOP
        == jnp.arange(sequences, dtype=jnp.int32)[:, None]
    ).astype(jnp.float32)


def here():
    return tuple(lax.axis_index(name) for name in EP_TP)


def ring_peer(step, z, y, x):
    return (z + step // 16) % 4, (y + (step // 4) % 4) % 4, (x + step % 4) % 4


def block_wait(ref, count, sem, device):
    return pltpu.make_async_remote_copy(
        src_ref=ref.at[pl.ds(0, count)],
        dst_ref=ref.at[pl.ds(0, count)],
        send_sem=sem,
        recv_sem=sem,
        device_id=device,
        device_id_type=MESH,
    )


def expert_kernel(
    blocks,
    mixer,
    after,
    gate_hbm,
    up_hbm,
    down_hbm,
    out,
    gate,
    up,
    down,
    arrived,
    wide,
    rows,
    hidden,
    leaving,
    returned,
    summed,
    load_sem,
    swap_send,
    swap_recv,
    out_send,
    out_recv,
    back_send,
    back_recv,
):
    z, y, x, c = here()
    me = (z * 4 + y) * 4 + x
    mine = pl.ds(pl.multiple_of(c * HID, 64), HID)
    weights = ((gate_hbm, gate), (up_hbm, up), (down_hbm, down))
    loads = [
        pltpu.make_async_copy(src, dst.at[mine], load_sem.at[i])
        for i, (src, dst) in enumerate(weights)
    ]
    for load in loads:
        load.start()
    twin = (z, y, x, 1 - c)
    barrier = pltpu.get_barrier_semaphore()

    def greet(step, carry):
        pz, py, px = ring_peer(step, z, y, x)
        pl.semaphore_signal(barrier, inc=1, device_id=(pz, py, px, c), device_id_type=MESH)
        return carry

    lax.fori_loop(1, 64, greet, 0)
    pl.semaphore_signal(barrier, inc=1, device_id=twin, device_id_type=MESH)
    pl.semaphore_wait(barrier, 64)

    def dispatch(step, carry):
        pz, py, px = ring_peer(step, z, y, x)
        pltpu.make_async_remote_copy(
            src_ref=blocks.at[2 * pz + py // 2],
            dst_ref=arrived.at[me],
            send_sem=out_send,
            recv_sem=out_recv,
            device_id=(pz, py, px, c),
            device_id_type=MESH,
        ).start()
        return carry

    lax.fori_loop(1, 64, dispatch, 0)
    swaps = [
        pltpu.make_async_remote_copy(
            src_ref=src,
            dst_ref=dst.at[mine],
            send_sem=swap_send.at[i],
            recv_sem=swap_recv.at[i],
            device_id=twin,
            device_id_type=MESH,
        )
        for i, (src, dst) in enumerate(weights)
    ]
    for swap in swaps:
        swap.start()
    arrived[me] = blocks[2 * z + y // 2]
    for load in loads:
        load.wait()
    block_wait(arrived, 63, out_recv, twin).wait_recv()

    def widen(s, carry):
        block = arrived[s].astype(F32)
        at = pl.ds(pl.multiple_of(s * 24, 8), 24)
        for j in range(4):
            wide[j, at, :] = block[:, j * 128 : (j + 1) * 128]
        return carry

    lax.fori_loop(0, 64, widen, 0)
    for q in range(8):
        for j in range(4):
            lane = q * 512 + j * 128
            rows[:, lane : lane + 128] = wide[j, pl.ds(q, 192, stride=8), :].astype(BF16)
    swaps[0].wait_recv()
    swaps[1].wait_recv()

    nt = (((1,), (1,)), ((), ()))

    def lift(half, carry):
        at = pl.ds(pl.multiple_of(half * HID, 64), HID)
        gated = lax.dot_general(rows[...], gate[at, :], nt, preferred_element_type=F32)
        upped = lax.dot_general(rows[...], up[at, :], nt, preferred_element_type=F32)
        hidden[half] = (jax.nn.silu(gated) * upped).astype(BF16)
        return carry

    lax.fori_loop(0, 2, lift, 0)
    swaps[2].wait_recv()

    def lower(q, carry):
        at = pl.ds(pl.multiple_of(q * 512, 512), 512)
        part = jnp.dot(hidden[0], down[0:HID, at], preferred_element_type=F32)
        part += jnp.dot(hidden[1], down[HID : 2 * HID, at], preferred_element_type=F32)
        for j in range(4):
            wide[j, pl.ds(q, 192, stride=8), :] = part[:, j * 128 : (j + 1) * 128]
        return carry

    lax.fori_loop(0, 8, lower, 0)

    def narrow(s, carry):
        at = pl.ds(pl.multiple_of(s * 24, 8), 24)
        leaving[s] = jnp.concatenate([wide[j, at, :] for j in range(4)], axis=1).astype(BF16)
        return carry

    lax.fori_loop(0, 64, narrow, 0)

    def give_back(step, carry):
        pz, py, px = ring_peer(step, z, y, x)
        pltpu.make_async_remote_copy(
            src_ref=leaving.at[(pz * 4 + py) * 4 + px],
            dst_ref=returned.at[me],
            send_sem=back_send,
            recv_sem=back_recv,
            device_id=(pz, py, px, c),
            device_id_type=MESH,
        ).start()
        return carry

    lax.fori_loop(1, 64, give_back, 0)
    returned[me] = leaving[me]
    block_wait(returned, 63, back_recv, twin).wait_recv()

    def total(e, carry):
        acc = returned[e * 8].astype(F32)
        for k in range(1, 8):
            acc += returned[e * 8 + k].astype(F32)
        summed[pl.ds(pl.multiple_of(e * 24, 8), 24), :] = acc
        return carry

    lax.fori_loop(0, EXPERTS, total, 0)
    routed = jnp.dot(
        mixer[...], summed[...], precision=lax.Precision.HIGHEST, preferred_element_type=F32
    )
    for q in range(8):
        lanes = slice(q * 512, (q + 1) * 512)
        out[:, lanes] = (after[:, lanes] + routed[q * 8 : (q + 1) * 8, :]).astype(BF16)
    for swap in swaps:
        swap.wait_send()
    block_wait(arrived, 63, out_send, twin).wait_send()
    block_wait(returned, 63, back_send, twin).wait_send()


def experts(blocks, mixer, after, gate_t, up_t, down):
    vmem = pl.BlockSpec(memory_space=pltpu.VMEM)
    hbm = pl.BlockSpec(memory_space=pl.ANY)
    dma = pltpu.SemaphoreType.DMA
    return pl.pallas_call(
        expert_kernel,
        out_shape=jax.ShapeDtypeStruct(after.shape, BF16),
        in_specs=[vmem, vmem, vmem, hbm, hbm, hbm],
        out_specs=vmem,
        scratch_shapes=[
            pltpu.VMEM((2 * HID, 4096), BF16),
            pltpu.VMEM((2 * HID, 4096), BF16),
            pltpu.VMEM((2 * HID, 4096), BF16),
            pltpu.VMEM((64, 24, 512), BF16),
            pltpu.VMEM((4, 1536, 128), F32),
            pltpu.VMEM((192, 4096), BF16),
            pltpu.VMEM((2, 192, HID), BF16),
            pltpu.VMEM((64, 24, 512), BF16),
            pltpu.VMEM((64, 24, 512), BF16),
            pltpu.VMEM((192, 512), F32),
            dma((3,)),
            dma((3,)),
            dma((3,)),
            dma,
            dma,
            dma,
            dma,
        ],
        compiler_params=pltpu.CompilerParams(
            collective_id=1, has_side_effects=True, vmem_limit_bytes=56 * 1024 * 1024
        ),
        name="experts",
    )(blocks, mixer, after, gate_t, up_t, down)


def attend_local(
    query_latents, query_rotary, latent_cache, rope_cache, new_latent, new_rope, lengths
):
    score_scale = (NOPE + ROPE) ** (-0.5)
    cache_scores = (
        jnp.einsum("shl,spl->shp", query_latents, latent_cache, preferred_element_type=jnp.float32)
        + jnp.einsum("shr,spr->shp", query_rotary, rope_cache, preferred_element_type=jnp.float32)
    ) * score_scale
    new_scores = (
        jnp.einsum("shl,sl->sh", query_latents, new_latent, preferred_element_type=jnp.float32)
        + jnp.einsum("shr,sr->sh", query_rotary, new_rope, preferred_element_type=jnp.float32)
    ) * score_scale
    visible = jnp.arange(latent_cache.shape[1], dtype=jnp.int32)[None, :] < lengths[:, None]
    cache_scores = jnp.where(visible[:, None, :], cache_scores, -jnp.inf)
    row_top = jnp.maximum(jnp.max(cache_scores, axis=-1), new_scores)
    cache_terms = jnp.exp(cache_scores - row_top[..., None])
    new_term = jnp.exp(new_scores - row_top)
    denominator = jnp.sum(cache_terms, axis=-1) + new_term
    cache_probs = (cache_terms / denominator[..., None]).astype(jnp.bfloat16)
    new_probs = (new_term / denominator).astype(jnp.bfloat16)
    mixture = jnp.einsum(
        "shp,spl->shl", cache_probs, latent_cache, preferred_element_type=jnp.float32
    )
    mixture = (
        mixture
        + new_probs.astype(jnp.float32)[..., None] * new_latent.astype(jnp.float32)[:, None, :]
    )
    return mixture.astype(jnp.bfloat16)


def local(
    residual,
    lengths,
    latent_cache,
    rope_cache,
    route_ids,
    route_scores,
    norm_first,
    norm_second,
    query_gain,
    latent_gain,
    query_down,
    latent_down,
    rope_down,
    query_latent,
    query_rope,
    value_up,
    output_weight,
    expert_gate,
    expert_up,
    expert_down,
):
    sequences = residual.shape[0]
    model_width = residual.shape[1]
    devices = lax.axis_size(EP_TP)
    stream = residual.astype(jnp.float32)
    normed = normalize(stream, norm_first).astype(jnp.bfloat16)
    slices = lax.all_to_all(normed, EP_TP, split_axis=1, concat_axis=0, tiled=True)
    query_width = query_down.shape[1]
    lowered = sum_by_axis(
        jnp.concatenate(
            [
                jnp.dot(slices, query_down, preferred_element_type=jnp.float32),
                jnp.dot(slices, latent_down, preferred_element_type=jnp.float32),
            ],
            axis=1,
        ),
        (("ep_0", "ep_1", "ep_2"), "tp"),
        0,
    )
    query_small = normalize(lowered[:, :query_width], query_gain).astype(jnp.bfloat16)
    new_latent = normalize(lowered[:, query_width:], latent_gain).astype(jnp.bfloat16)
    turns = rotary_angles(lengths, rope_down.shape[1])
    new_rope = rotate(jnp.dot(normed, rope_down, preferred_element_type=jnp.float32), turns).astype(
        jnp.bfloat16
    )
    latent_columns = query_latent.shape[1]
    shard_rows = gathered_by_axis(query_small, (("ep_0", "ep_1", "ep_2"), "tp"), 0)
    columns = jnp.concatenate(
        [
            jnp.dot(shard_rows, query_latent, preferred_element_type=jnp.float32),
            jnp.dot(shard_rows, query_rope, preferred_element_type=jnp.float32),
        ],
        axis=1,
    ).astype(jnp.bfloat16)
    at_home = lax.all_to_all(columns, EP_TP, split_axis=0, concat_axis=1, tiled=True)
    at_home = at_home.reshape(sequences, devices, columns.shape[1])
    head_count = value_up.shape[1]
    query_latents = at_home[:, :, :latent_columns].reshape(sequences, head_count, -1)
    query_pe = at_home[:, :, latent_columns:].reshape(sequences, head_count, -1)
    query_rotary = rotate(query_pe.astype(jnp.float32), turns[:, None, :]).astype(jnp.bfloat16)
    mixture = attend_local(
        query_latents, query_rotary, latent_cache, rope_cache, new_latent, new_rope, lengths
    )
    values = jnp.einsum("shl,lhv->shv", mixture, value_up, preferred_element_type=jnp.float32)
    values = values.astype(jnp.bfloat16).reshape(sequences, -1)
    output_cols = jnp.dot(
        lax.all_gather(values, EP_TP, axis=0, tiled=True),
        output_weight,
        preferred_element_type=jnp.float32,
    ).astype(jnp.bfloat16)
    attended = lax.all_to_all(output_cols, EP_TP, split_axis=0, concat_axis=1, tiled=True)
    after_attention = stream + attended.astype(jnp.float32)
    second = normalize(after_attention, norm_second).astype(jnp.bfloat16)
    owners = owner_table(sequences)
    assign = sequences * TOP
    weights = jax.nn.softmax(route_scores.astype(jnp.float32), axis=-1)
    matches = slot_tables(route_ids.reshape(1, assign))[0].astype(jnp.float32)
    picker = jnp.einsum("aec,sa->ecs", matches, owners).astype(jnp.bfloat16)
    outbound = jnp.einsum("ecs,sd->ecd", picker, second, preferred_element_type=jnp.float32).astype(
        jnp.bfloat16
    )
    blocks = outbound.reshape(EXPERTS, CAP * 8, model_width // 8)
    combine_weights = matches * weights.reshape(assign)[:, None, None]
    token_weights = jnp.einsum("aec,sa->sec", combine_weights, owners, precision="highest")
    mixer = jnp.einsum("ter,qp->qterp", token_weights, jnp.eye(8, dtype=F32)).reshape(64, 192)
    layer_out = experts(
        blocks, mixer, after_attention, expert_gate.T, expert_up.T, expert_down
    )
    return (layer_out, new_latent, new_rope)


def solution(mesh):
    torus = Mesh(mesh.devices.reshape(4, 4, 4, mesh.shape["tp"]), ("ep_0", "ep_1", "ep_2", "tp"))
    placed = (
        P(EP_TP, None),
        P(EP_TP),
        P(EP_TP, None, None),
        P(EP_TP, None, None),
        P(EP_TP, None),
        P(EP_TP, None),
        P(),
        P(),
        P(),
        P(),
        P(EP_TP, None),
        P(EP_TP, None),
        P(),
        P(None, EP_TP),
        P(None, EP_TP),
        P(),
        P(None, EP_TP),
        P(None, EP_TP),
        P(None, EP_TP),
        P(EP_TP, None),
    )
    return jax.shard_map(
        local,
        mesh=torus,
        in_specs=placed,
        out_specs=(P(EP_TP, None), P(EP_TP, None), P(EP_TP, None)),
        check_vma=False,
    )
```
